128 devices in a mesh: fs: 16 (over z, x), tp: 8 (over y, core).
Axes of the slice: x: 4, y: 4, z: 4, core: 2. Of those that a mesh axis runs over, the one named last changes fastest.
Arguments:
- layer_inputs: bfloat16 [40960, 2048], P('fs'), may hold values from -6 to 6
- output_cot: bfloat16 [40960, 2048], P('fs'), may hold values from -6 to 6
- query_cot: bfloat16 [40960, 2048], P('fs', 'tp'), may hold values from -6 to 6
- head_outputs: bfloat16 [40960, 2048], P('fs', 'tp'), may hold values from -6 to 6
- weights: float32 [2, 2048, 2048], P(None, 'fs', 'tp'), may hold values from -0.125 to 0.125
- factors: bfloat16 [2, 2048, 256], replicated, may hold values from -0.125 to 0.125
- first_moment: float32 [2, 256, 2048], P(None, None, 'tp'), may hold values from -600 to 600
- second_moment: float32 [2, 256, 2048], P(None, None, 'tp'), may hold values from 1000 to 100000
Outputs:
- new_weights: float32 [2, 2048, 2048], P(None, 'fs', 'tp')
- update: float32 [2, 2048, 2048], P(None, 'fs', 'tp')
- new_first: float32 [2, 256, 2048], P(None, None, 'tp')
- new_second: float32 [2, 256, 2048], P(None, None, 'tp')
- weight_copy: bfloat16 [2, 2048, 2048], P(None, None, 'tp')
The draws below stay inside these ranges and needn't reach their ends.
All inputs are finite; a program needn't handle non-finite values.
Results may differ from the reference program's by a relative error of at most 0.00055.
Values may be sent and summed in bfloat16 or wider, within the bound.
No kernel may reach another device: no remote copies, remote signals or barrier semaphores. Data moves between devices by JAX's collectives and lax.ppermute only.
A program may use at most 128 MiB of HBM per device.

```python
import math
import jax
import jax.numpy as jnp
from jax import lax

D = 2048
QDIM = 2048
RANK = 256
TOKENS = 40960


def block_scale(own_key, shape, split, smallest, high):
    def one(dim, blocks):
        steps = jax.random.uniform(jax.random.fold_in(jax.random.fold_in(own_key, 6), dim), (blocks,), jnp.float32, smallest / len(split), high / len(split))
        return jnp.repeat(jnp.exp(steps), shape[dim] // blocks).reshape((-1,) + (1,) * (len(shape) - dim - 1))

    loudness = one(*split[0])
    for cut in split[1:]:
        loudness = loudness * one(*cut)
    return loudness


def noise(own_key, extent, spread, reach, cuts=(), kind=jnp.bfloat16):
    result = spread * jax.random.normal(own_key, extent, jnp.float32)
    if cuts:
        result = result * block_scale(own_key, extent, cuts, -0.22, 0.18)
    return jnp.clip(result, -reach, reach).astype(kind)


def setup_inputs(seed: int = 0) -> dict:
    streams_of = jax.random.split(jax.random.key(seed), 9)
    return {
        "layer_inputs": noise(streams_of[0], (TOKENS, D), 1.0, 6.0, ((0, 16),)),
        "output_cot": noise(streams_of[1], (TOKENS, D), 1.0, 6.0, ((0, 16),)),
        "query_cot": noise(streams_of[2], (TOKENS, QDIM), 1.0, 6.0, ((0, 16), (1, 8))),
        "head_outputs": noise(streams_of[3], (TOKENS, QDIM), 1.0, 6.0, ((0, 16), (1, 8))),
        "weights": noise(streams_of[4], (2, D, QDIM), D ** -0.5, 0.125, ((1, 16), (2, 8)), jnp.float32),
        "factors": noise(streams_of[5], (2, D, RANK), D ** -0.5, 0.125),
        "first_moment": noise(streams_of[6], (2, RANK, QDIM), 100.0, 600.0, ((2, 8),), jnp.float32),
        "second_moment": jnp.clip(jnp.exp(math.log(100000.0) - 4.6051702 * jax.random.uniform(streams_of[7], (2, RANK, QDIM), jnp.float32) ** block_scale(streams_of[7], (2, RANK, QDIM), ((2, 8),), -0.2, 0.2)), 1000.0, 100000.0),
    }


def reference(layer_inputs, output_cot, query_cot, head_outputs, weights, factors, first_moment, second_moment):
    lefts = (layer_inputs, output_cot)
    rights = (query_cot, head_outputs)
    steps = []
    firsts = []
    seconds = []
    for index in range(2):
        grad = jnp.dot(lefts[index].T, rights[index], preferred_element_type=jnp.float32)
        factor = factors[index].astype(jnp.float32)
        low = jnp.dot(factor.T, grad, precision=lax.Precision.HIGHEST)
        first = 0.9 * first_moment[index] + 0.1 * low
        second = 0.95 * second_moment[index] + 0.05 * low * low
        normed = first / (jnp.sqrt(second) + 1e-06)
        ratio = jnp.sqrt(jnp.sum(normed * normed)) / jnp.sqrt(jnp.sum(low * low) + 1e-06)
        resid = grad - jnp.dot(factor, low, precision=lax.Precision.HIGHEST)
        steps.append(jnp.dot(factor, normed, precision=lax.Precision.HIGHEST) + ratio * resid)
        firsts.append(first)
        seconds.append(second)
    step = jnp.stack(steps)
    update = step * lax.rsqrt(jnp.mean(step * step) + 1e-06)
    new_weights = weights - 0.02 * update
    return (new_weights, update, jnp.stack(firsts), jnp.stack(seconds), new_weights.astype(jnp.bfloat16))
```

```python
import itertools

import jax
import jax.numpy as jnp
from jax import lax
from jax.experimental import pallas as pl
from jax.experimental.pallas import tpu as pltpu
from jax.sharding import Mesh
from jax.sharding import PartitionSpec as P

D = 2048
QDIM = 2048
FS = ("fs_0", "fs_1")
ALL = ("fs_0", "fs_1", "tp_0", "tp_1")
SIZES = (4, 4, 4, 2)
TURNS = (2, 1, 3, 0)
HIGHEST = lax.Precision.HIGHEST


def pairs_along(first, offset):
    pairs = []
    for place in itertools.product(*(range(size) for size in SIZES)):
        there = list(place)
        axis = 1 if (place[3] == 0) == first else 0
        there[axis] = (there[axis] + offset) % 4
        flat = [((a * 4 + b) * 4 + c) * 2 + d for a, b, c, d in (place, there)]
        pairs.append(tuple(flat))
    return pairs


def moved(array, first, offset):
    return lax.ppermute(array, ALL, pairs_along(first, offset))


def grad_kernel(order, *refs):
    lefts, right, factors = refs[:4], refs[4], refs[5:9]
    grad_ref, low_ref = refs[9:]
    low = None
    for j in range(4):
        grad = lax.dot_general(
            lefts[j][...],
            right[...],
            (((0,), (0,)), ((), ())),
            preferred_element_type=jnp.float32,
        )
        grad_ref[0, j] = grad
        high = grad.astype(jnp.bfloat16)
        rest = (grad - high.astype(jnp.float32)).astype(jnp.bfloat16)
        for piece in (high, rest):
            term = lax.dot_general(
                factors[j][0],
                piece,
                (((0,), (0,)), ((), ())),
                preferred_element_type=jnp.float32,
            )
            low = term if low is None else low + term

    @pl.when(pl.program_id(0) == 0)
    def _():
        low_ref[...] = low

    @pl.when(pl.program_id(0) > 0)
    def _():
        low_ref[...] += low


def grads_of(order, left, right, factors, index):
    tokens, width = right.shape
    rank = factors.shape[2]
    rows = D // 16

    def left_spec(j):
        return pl.BlockSpec((tokens, rows), lambda i, order: (0, order[4 * i + j]))

    def factor_spec(j):
        return pl.BlockSpec(
            (1, rows, rank), lambda i, order: (index, order[4 * i + j], 0)
        )

    return pl.pallas_call(
        grad_kernel,
        grid_spec=pltpu.PrefetchScalarGridSpec(
            num_scalar_prefetch=1,
            grid=(4,),
            in_specs=[left_spec(j) for j in range(4)]
            + [pl.BlockSpec((tokens, width), lambda i, order: (0, 0))]
            + [factor_spec(j) for j in range(4)],
            out_specs=[
                pl.BlockSpec((1, 4, rows, width), lambda i, order: (i, 0, 0, 0)),
                pl.BlockSpec((rank, width), lambda i, order: (0, 0)),
            ],
        ),
        out_shape=[
            jax.ShapeDtypeStruct((4, 4, rows, width), jnp.float32),
            jax.ShapeDtypeStruct((rank, width), jnp.float32),
        ],
        compiler_params=pltpu.CompilerParams(vmem_limit_bytes=20 * 2**20),
        cost_estimate=pl.CostEstimate(
            flops=2 * tokens * D * width + 4 * D * rank * width,
            bytes_accessed=2 * tokens * (D + width) + 4 * D * width,
            transcendentals=0,
        ),
    )(order, *[left] * 4, right, *[factors] * 4)


def place_kernel(order, *refs):
    pieces, out, sems = refs[:4], refs[4], refs[5]
    copies = []
    for q in range(4):
        for k in range(2):
            for j in range(4):
                start = pl.multiple_of(order[4 * j + q] * 128, 128)
                copies.append(
                    pltpu.make_async_copy(
                        pieces[q].at[k, j],
                        out.at[k, pl.ds(start, 128)],
                        sems.at[q, k, j],
                    )
                )
    for copy in copies:
        copy.start()
    for copy in copies:
        copy.wait()


def placed(order, pieces):
    width = pieces[0].shape[-1]
    return pl.pallas_call(
        place_kernel,
        grid_spec=pltpu.PrefetchScalarGridSpec(
            num_scalar_prefetch=1,
            grid=(),
            in_specs=[pl.BlockSpec(memory_space=pltpu.VMEM)] * 4,
            out_specs=pl.BlockSpec(memory_space=pl.ANY),
            scratch_shapes=[pltpu.SemaphoreType.DMA((4, 2, 4))],
        ),
        out_shape=jax.ShapeDtypeStruct((2, D, width), jnp.bfloat16),
        compiler_params=pltpu.CompilerParams(vmem_limit_bytes=16 * 2**20),
    )(order, *pieces)


def per_device(
    layer_inputs, output_cot, query_cot, head_outputs, weights, factors, first_moment, second_moment
):
    z, x, core = (lax.axis_index(a) for a in ("fs_0", "fs_1", "tp_1"))
    along = jnp.where(core == 0, x, z)
    across = jnp.where(core == 0, z, x)
    steps = jnp.arange(4)
    firsts_at = (along + steps)[:, None] % 4
    seconds_at = (across + steps)[None, :] % 4
    order = jnp.where(core == 0, seconds_at * 4 + firsts_at, firsts_at * 4 + seconds_at)
    order = order.astype(jnp.int32)
    turned = order[jnp.array(TURNS)].reshape(-1)
    flat_order = order.reshape(-1)

    lefts = (layer_inputs, output_cot)
    rights = (query_cot, head_outputs)
    lows, sums = [], []
    for k in range(2):
        grads, low = grads_of(turned, lefts[k], rights[k], factors, k)
        lows.append(low)
        far, ahead, behind, own = grads
        got_a = moved(far[:2], True, 1)
        got_b = moved(far[2:], True, -1)
        ahead = jnp.concatenate([ahead[:2] + got_a, ahead[2:]])
        behind = jnp.concatenate([behind[:2], behind[2:] + got_b])
        sums.append(own + moved(ahead, True, 1) + moved(behind, True, -1))
    sums = jnp.stack(sums)
    grad = sums[:, 0]
    for offset in (1, 3, 2):
        grad = grad + moved(sums[:, offset], False, offset)

    low = jnp.stack(lows)
    rank, width = low.shape[1:]
    pieces = jnp.moveaxis(low.reshape(2, 16, rank // 16, width), 1, 0)
    part = lax.all_to_all(pieces, FS, split_axis=0, concat_axis=0, tiled=True).sum(axis=0)
    copies = jnp.broadcast_to(part, (16, *part.shape))
    low = lax.all_to_all(copies, FS, split_axis=0, concat_axis=0, tiled=True)
    low = jnp.moveaxis(low, 0, 1).reshape(2, rank, width)

    first = 0.9 * first_moment + 0.1 * low
    second = 0.95 * second_moment + 0.05 * low * low
    normed = first / (jnp.sqrt(second) + 1e-06)

    near = factors.reshape(2, 16, D // 16, rank)[:, order[:, 0]].astype(jnp.float32)
    lifted = jnp.einsum("kjdr,krq->kjdq", near, normed, precision=HIGHEST)
    fitted = jnp.einsum("kjdr,krq->kjdq", near, low, precision=HIGHEST)
    resid = grad - fitted[:, 0]

    def total_of(array):
        return jnp.sum(array, axis=tuple(range(1, array.ndim)))

    scalars = jnp.concatenate(
        [
            total_of(lifted[:, 0] * lifted[:, 0]),
            total_of(lifted[:, 0] * resid),
            total_of(resid * resid),
            total_of(normed * normed) / 16.0,
            total_of(low * low) / 16.0,
        ]
    )
    scalars = jnp.broadcast_to(scalars, (128, 10))
    scalars = lax.all_to_all(scalars, ALL, split_axis=0, concat_axis=0, tiled=True)
    flat, cross, square, norms, lengths = scalars.sum(axis=0).reshape(5, 2)
    ratio = jnp.sqrt(norms) / jnp.sqrt(lengths + 1e-06)
    total = jnp.sum(flat + 2.0 * ratio * cross + ratio * ratio * square)
    scale = lax.rsqrt(jnp.maximum(total, 0.0) / (2.0 * D * QDIM) + 1e-06)

    both = jnp.stack([grad, weights])
    all_grads, all_weights = jnp.stack(
        [both] + [moved(both, True, -offset) for offset in (1, 2, 3)], axis=2
    )
    update = scale * (lifted + ratio[:, None, None, None] * (all_grads - fitted))
    new_weights = all_weights - 0.02 * update
    copy = new_weights.astype(jnp.bfloat16)
    pieces = [copy] + [moved(copy, False, -offset) for offset in (1, 2, 3)]
    weight_copy = placed(flat_order, pieces)
    return (new_weights[:, 0], update[:, 0], first, second, weight_copy)


def solution(mesh):
    finer = Mesh(mesh.devices.reshape(SIZES), ALL)
    tp = ("tp_0", "tp_1")
    in_specs = (
        P(FS, None),
        P(FS, None),
        P(FS, tp),
        P(FS, tp),
        P(None, FS, tp),
        P(),
        P(None, None, tp),
        P(None, None, tp),
    )
    out_specs = (
        P(None, FS, tp),
        P(None, FS, tp),
        P(None, None, tp),
        P(None, None, tp),
        P(None, None, tp),
    )
    return jax.shard_map(
        per_device, mesh=finer, in_specs=in_specs, out_specs=out_specs, check_vma=False
    )
```

```python
import functools
import itertools

import jax
import jax.numpy as jnp
from jax import lax
from jax.experimental import pallas as pl
from jax.experimental.pallas import tpu as pltpu
from jax.sharding import Mesh
from jax.sharding import PartitionSpec as P

D = 2048
QDIM = 2048
ROWS = 128
LOW_ROWS = 16
FS = ("fs_0", "fs_1")
ALL = ("fs_0", "fs_1", "tp_0", "tp_1")
SIZES = (4, 4, 4, 2)


def pairs_along(first, offset):
    pairs = []
    for place in itertools.product(*(range(size) for size in SIZES)):
        there = list(place)
        axis = 1 if (place[3] == 0) == first else 0
        there[axis] = (there[axis] + offset) % 4
        flat = [((a * 4 + b) * 4 + c) * 2 + d for a, b, c, d in (place, there)]
        pairs.append(tuple(flat))
    return pairs


def moved(array, first, offset):
    return lax.ppermute(array, ALL, pairs_along(first, offset))


def small_call(kernel, shapes, prefetched=(), aliases={}, kind=None):
    def call(*arrays):
        return pl.pallas_call(
            kernel,
            grid_spec=pltpu.PrefetchScalarGridSpec(
                num_scalar_prefetch=len(prefetched),
                grid=(),
                in_specs=[pl.BlockSpec(memory_space=pltpu.VMEM)] * len(arrays),
                out_specs=[pl.BlockSpec(memory_space=pltpu.VMEM)] * len(shapes),
            ),
            out_shape=[jax.ShapeDtypeStruct(s, jnp.float32) for s in shapes],
            input_output_aliases=aliases,
            compiler_params=pltpu.CompilerParams(vmem_limit_bytes=16 * 2**20),
        )(*prefetched, *arrays)

    return call


def rows_of(ref, block, rows):
    return ref[pl.ds(pl.multiple_of(block * rows, rows), rows), :]


def spread_kernel(order, places, grad, low, far_a, far_b, ahead, behind, own):
    def fill(out, slot, along, across):
        at = 4 * along + across
        out[slot, :ROWS] = rows_of(grad, order[at], ROWS)
        out[slot, ROWS:] = rows_of(low, places[at], LOW_ROWS)

    for j in range(4):
        fill(own, j, 0, j)
        fill(ahead, j, 1, j)
        fill(behind, j, 3, j)
    for j in range(2):
        fill(far_a, j, 2, j)
        fill(far_b, j, 2, 2 + j)


def add_kernel(offset, base, more, out):
    count = more.shape[0]
    out[offset : offset + count] = base[offset : offset + count] + more[...]


def join_kernel(*refs):
    ins, outs, low = refs[:6], refs[6:10], refs[10]
    for k in range(2):
        own, left, right = ins[3 * k : 3 * k + 3]
        for j in range(4):
            total = own[j] + left[j] + right[j]
            outs[j][k] = total[:ROWS]
            low[k, LOW_ROWS * j : LOW_ROWS * (j + 1)] = total[ROWS:]


def sum_kernel(own, ahead, far, behind, total):
    total[...] = (own[...] + ahead[...]) + (far[...] + behind[...])


def grad_kernel(own, ahead, far, behind, weights, both):
    both[0] = (own[...] + ahead[...]) + (far[...] + behind[...])
    both[1] = weights[...]


def three(array):
    pieces = []
    for _ in range(3):
        piece = array.astype(jnp.bfloat16)
        pieces.append(piece)
        array = array - piece.astype(jnp.float32)
    return pieces


def moment_kernel(order, places, *refs):
    quarters, factors, first_in, second_in = refs[:4], refs[4], refs[5], refs[6]
    first_out, second_out, lifted, fitted, norms, low = refs[7:]
    for k in range(2):
        for a in range(4):
            for j in range(4):
                start = pl.multiple_of(places[4 * a + j] * LOW_ROWS, LOW_ROWS)
                low[k, pl.ds(start, LOW_ROWS)] = quarters[a][
                    k, LOW_ROWS * j : LOW_ROWS * (j + 1)
                ]
        lows = low[k]
        first = 0.9 * first_in[k] + 0.1 * lows
        second = 0.95 * second_in[k] + 0.05 * lows * lows
        first_out[k] = first
        second_out[k] = second
        normed = first / (jnp.sqrt(second) + 1e-06)
        norms[k] = jnp.sum(normed * normed, axis=0, keepdims=True)
        norms[2 + k] = jnp.sum(lows * lows, axis=0, keepdims=True)
        pairs = ((lifted, three(normed)), (fitted, three(lows)))
        for a in range(4):
            near = rows_of(factors.at[k], order[4 * a], ROWS)
            for out, pieces in pairs:
                out[k, a] = sum(
                    jnp.dot(near, piece, preferred_element_type=jnp.float32)
                    for piece in reversed(pieces)
                )


def resid_kernel(both, lifted, fitted, sums):
    for k in range(2):
        lift = lifted[k, 0]
        resid = both[0, k] - fitted[k, 0]
        sums[k] = jnp.sum(lift * lift, axis=0, keepdims=True)
        sums[2 + k] = jnp.sum(lift * resid, axis=0, keepdims=True)
        sums[4 + k] = jnp.sum(resid * resid, axis=0, keepdims=True)


def products(left, right, factor):
    grad = lax.dot_general(
        left, right, (((0,), (0,)), ((), ())), preferred_element_type=jnp.float32
    )
    high = grad.astype(jnp.bfloat16)
    restored = lax.optimization_barrier(high).astype(jnp.float32)
    rest = (grad - restored).astype(jnp.bfloat16)
    low = 0.0
    for piece in (high, rest):
        low = low + lax.dot_general(
            factor, piece, (((0,), (0,)), ((), ())), preferred_element_type=jnp.float32
        )
    return grad, low


def place_kernel(across, *refs):
    order, pieces, out, sems = refs[0], refs[1 : 1 + len(across)], refs[-2], refs[-1]
    copies = []
    for n, q in enumerate(across):
        for k in range(2):
            for j in range(4):
                start = pl.multiple_of(order[4 * j + q] * ROWS, ROWS)
                copies.append(
                    pltpu.make_async_copy(
                        pieces[n].at[k, j], out.at[k, pl.ds(start, ROWS)], sems.at[n, k, j]
                    )
                )
    for copy in copies:
        copy.start()
    for copy in copies:
        copy.wait()


def placed(order, across, pieces, out=None):
    count = len(across)
    olds = [] if out is None else [out]
    width = pieces[0].shape[-1]
    return pl.pallas_call(
        functools.partial(place_kernel, across),
        grid_spec=pltpu.PrefetchScalarGridSpec(
            num_scalar_prefetch=1,
            grid=(),
            in_specs=[pl.BlockSpec(memory_space=pltpu.VMEM)] * count
            + [pl.BlockSpec(memory_space=pl.ANY)] * len(olds),
            out_specs=pl.BlockSpec(memory_space=pl.ANY),
            scratch_shapes=[pltpu.SemaphoreType.DMA((count, 2, 4))],
        ),
        out_shape=jax.ShapeDtypeStruct((2, D, width), jnp.bfloat16),
        input_output_aliases={1 + count: 0} if olds else {},
        compiler_params=pltpu.CompilerParams(vmem_limit_bytes=8 * 2**20),
    )(order, *pieces, *olds)


def per_device(
    layer_inputs, output_cot, query_cot, head_outputs, weights, factors, first_moment, second_moment
):
    z, x, core = (lax.axis_index(a) for a in ("fs_0", "fs_1", "tp_1"))
    along = jnp.where(core == 0, x, z)
    across = jnp.where(core == 0, z, x)
    steps = jnp.arange(16, dtype=jnp.int32)
    there = (along + steps // 4) % 4
    beyond = (across + steps % 4) % 4
    order = jnp.where(core == 0, beyond * 4 + there, there * 4 + beyond)
    places = jnp.where(core == 0, steps % 4 * 4 + there, there * 4 + steps % 4)
    orders = (order, places)

    lefts = (layer_inputs, output_cot)
    rights = (query_cot, head_outputs)
    width = weights.shape[2]
    deep = ROWS + LOW_ROWS
    full, half = (4, deep, width), (2, deep, width)
    parts = []
    for k in range(2):
        grads, low = products(lefts[k], rights[k], factors[k])
        far_a, far_b, ahead, behind, own = small_call(
            spread_kernel, (half, half, full, full, full), orders
        )(grads, low)
        add_a, add_b = (functools.partial(add_kernel, offset) for offset in (0, 2))
        (ahead,) = small_call(add_a, (full,), aliases={0: 0})(ahead, moved(far_a, True, 1))
        (behind,) = small_call(add_b, (full,), aliases={0: 0})(behind, moved(far_b, True, -1))
        parts += [own, moved(ahead, True, 1), moved(behind, True, -1)]
    block, flat = (2, ROWS, width), (2, 4 * LOW_ROWS, width)
    own, ahead, far, behind, low = small_call(join_kernel, (block,) * 4 + (flat,))(*parts)
    (quarter,) = small_call(sum_kernel, (flat,))(
        low, moved(low, False, 1), moved(low, False, 2), moved(low, False, -1)
    )
    quarters = [quarter] + [moved(quarter, True, -offset) for offset in (1, 2, 3)]
    (both,) = small_call(grad_kernel, ((2, *block),))(
        own, moved(ahead, False, 1), moved(far, False, 2), moved(behind, False, -1), weights
    )

    rank = factors.shape[2]
    square, near = (2, rank, width), (2, 4, ROWS, width)
    first, second, lifted, fitted, norms, _ = small_call(
        moment_kernel, (square, square, near, near, (4, 1, width), square), orders
    )(*quarters, factors, first_moment, second_moment)
    (sums,) = small_call(resid_kernel, ((6, 1, width),))(both, lifted, fitted)

    scalars = jnp.concatenate([jnp.sum(sums, axis=(1, 2)), jnp.sum(norms, axis=(1, 2)) / 16.0])
    scalars = jnp.broadcast_to(scalars, (128, 10))
    scalars = lax.all_to_all(scalars, ALL, split_axis=0, concat_axis=0, tiled=True)
    flat, cross, square, norms, lengths = scalars.sum(axis=0).reshape(5, 2)
    ratio = jnp.sqrt(norms) / jnp.sqrt(lengths + 1e-06)
    total = jnp.sum(flat + 2.0 * ratio * cross + ratio * ratio * square)
    scale = lax.rsqrt(jnp.maximum(total, 0.0) / (2.0 * D * QDIM) + 1e-06)

    near = [both] + [moved(both, True, -offset) for offset in (1, 2, 3)]
    all_grads, all_weights = jnp.stack(near, axis=2)

    def stepped(lifted, fitted, grads, weights):
        ratios = ratio.reshape(2, *[1] * (grads.ndim - 1))
        update = scale * (lifted + ratios * (grads - fitted))
        return update, weights - 0.02 * update

    copy = stepped(lifted, fitted, all_grads, all_weights)[1].astype(jnp.bfloat16)
    update, new_weights = stepped(lifted[:, 0], fitted[:, 0], both[0], weights)
    pieces = [copy] + [moved(copy, False, -offset) for offset in (1, 2, 3)]
    weight_copy = placed(order, (0,), pieces[:1])
    weight_copy = placed(order, (1, 3), pieces[1::2], weight_copy)
    weight_copy = placed(order, (2,), pieces[2:3], weight_copy)
    return (new_weights, update, first, second, weight_copy)


def solution(mesh):
    finer = Mesh(mesh.devices.reshape(SIZES), ALL)
    tp = ("tp_0", "tp_1")
    in_specs = (
        P(FS, None),
        P(FS, None),
        P(FS, tp),
        P(FS, tp),
        P(None, FS, tp),
        P(),
        P(None, None, tp),
        P(None, None, tp),
    )
    out_specs = (
        P(None, FS, tp),
        P(None, FS, tp),
        P(None, None, tp),
        P(None, None, tp),
        P(None, None, tp),
    )
    return jax.shard_map(
        per_device, mesh=finer, in_specs=in_specs, out_specs=out_specs, check_vma=False
    )
```

```python
import functools
import itertools

import jax
import jax.numpy as jnp
from jax import lax
from jax.experimental import pallas as pl
from jax.experimental.pallas import tpu as pltpu
from jax.sharding import Mesh
from jax.sharding import PartitionSpec as P


D = 2048
QDIM = 2048
ROWS = 128
LOW_ROWS = 16
FS = ("fs_0", "fs_1")
ALL = ("fs_0", "fs_1", "tp_0", "tp_1")
SIZES = (4, 4, 4, 2)


def pairs_along(first, offset):
    pairs = []
    for place in itertools.product(*(range(size) for size in SIZES)):
        there = list(place)
        axis = 1 if (place[3] == 0) == first else 0
        there[axis] = (there[axis] + offset) % 4
        flat = [((a * 4 + b) * 4 + c) * 2 + d for a, b, c, d in (place, there)]
        pairs.append(tuple(flat))
    return pairs


def moved(array, first, offset):
    return lax.ppermute(array, ALL, pairs_along(first, offset))


def to_all(array, first, sign=1):
    return [moved(array[n], first, sign * (n + 1)) for n in range(3)]


def small_call(kernel, shapes, prefetched=(), aliases={}):
    def call(*arrays):
        return pl.pallas_call(
            kernel,
            grid_spec=pltpu.PrefetchScalarGridSpec(
                num_scalar_prefetch=len(prefetched),
                grid=(),
                in_specs=[pl.BlockSpec(memory_space=pltpu.VMEM)] * len(arrays),
                out_specs=[pl.BlockSpec(memory_space=pltpu.VMEM)] * len(shapes),
            ),
            out_shape=[jax.ShapeDtypeStruct(s, jnp.float32) for s in shapes],
            input_output_aliases=aliases,
            compiler_params=pltpu.CompilerParams(vmem_limit_bytes=8 * 2**20),
        )(*prefetched, *arrays)

    return call


def rows_of(ref, block, rows):
    return ref[pl.ds(pl.multiple_of(block * rows, rows), rows), :]


def spread_kernel(order, grad, *outs):
    for along, out in enumerate(outs):
        for j in range(4):
            out[j] = rows_of(grad, order[4 * along + j], ROWS)


def spread_low_kernel(places, low_0, low_1, *outs):
    for along, out in enumerate(outs):
        for k, low in enumerate((low_0, low_1)):
            for j in range(4):
                out[j, LOW_ROWS * k : LOW_ROWS * (k + 1)] = rows_of(
                    low, places[4 * along + j], LOW_ROWS
                )


def add_kernel(base, more, out):
    out[...] = base[...] + more[...]


def join_kernel(*refs):
    ins, outs = refs[:6], refs[6:]
    for k in range(2):
        own, left, right = ins[3 * k : 3 * k + 3]
        for j in range(4):
            outs[j][k] = own[j] + left[j] + right[j]


def sum_kernel(own, ahead, far, behind, total):
    total[...] = (own[...] + ahead[...]) + (far[...] + behind[...])


def three(array):
    pieces = []
    for _ in range(3):
        piece = array.astype(jnp.bfloat16)
        pieces.append(piece)
        array = array - piece.astype(jnp.float32)
    return pieces


def moment_kernel(order, places, *refs):
    quarters, factors, first_in, second_in = refs[:4], refs[4], refs[5], refs[6]
    first_out, second_out, norms, lift_own, fit_own, lifted, fitted = refs[7:14]
    low, lift, fit, sems = refs[14:]
    copies = []
    for k in range(2):
        for a in range(4):
            for j in range(4):
                start = pl.multiple_of(places[4 * a + j] * LOW_ROWS, LOW_ROWS)
                low[k, pl.ds(start, LOW_ROWS)] = quarters[a][
                    j, LOW_ROWS * k : LOW_ROWS * (k + 1)
                ]
    for k in range(2):
        lows = low[k]
        first = 0.9 * first_in[k] + 0.1 * lows
        second = 0.95 * second_in[k] + 0.05 * lows * lows
        first_out[k] = first
        second_out[k] = second
        normed = first / (jnp.sqrt(second) + 1e-06)
        norms[k] = jnp.sum(normed * normed, axis=0, keepdims=True)
        norms[2 + k] = jnp.sum(lows * lows, axis=0, keepdims=True)
        near = jnp.concatenate(
            [rows_of(factors.at[k], order[4 * a], ROWS) for a in range(4)], axis=0
        )
        for n, (array, buffer, own, out) in enumerate(
            ((normed, lift, lift_own, lifted), (lows, fit, fit_own, fitted))
        ):
            value = sum(
                jnp.dot(near, piece, preferred_element_type=jnp.float32)
                for piece in reversed(three(array))
            )
            buffer[k] = value.reshape(buffer.shape[1:])
            own[k] = value[:ROWS]
            copies.append(pltpu.make_async_copy(buffer.at[k], out.at[k], sems.at[k, n]))
    for copy in copies:
        copy.start()
    for copy in copies:
        copy.wait()


def moments(orders, quarters, factors, first_moment, second_moment):
    rank, width = first_moment.shape[1:]
    square, block, near = (2, rank, width), (2, ROWS, width), (2, 4, ROWS, width)
    shapes = (square, square, (4, 1, width), block, block, near, near)
    return pl.pallas_call(
        moment_kernel,
        grid_spec=pltpu.PrefetchScalarGridSpec(
            num_scalar_prefetch=2,
            grid=(),
            in_specs=[pl.BlockSpec(memory_space=pltpu.VMEM)] * 7,
            out_specs=[pl.BlockSpec(memory_space=pltpu.VMEM)] * 5
            + [pl.BlockSpec(memory_space=pltpu.HBM)] * 2,
            scratch_shapes=[
                pltpu.VMEM(square, jnp.float32),
                pltpu.VMEM(near, jnp.float32),
                pltpu.VMEM(near, jnp.float32),
                pltpu.SemaphoreType.DMA((2, 2)),
            ],
        ),
        out_shape=[jax.ShapeDtypeStruct(s, jnp.float32) for s in shapes],
        compiler_params=pltpu.CompilerParams(vmem_limit_bytes=20 * 2**20),
    )(*orders, *quarters, factors, first_moment, second_moment)


def finish_kernel(own, ahead, far, behind, weights, lifted, fitted, norms, row, both, buffer, sem):
    grad = (own[...] + ahead[...]) + (far[...] + behind[...])
    buffer[0] = grad
    buffer[1] = weights[...]
    terms = [[], [], [], [], []]
    for k in range(2):
        lift = lifted[k]
        resid = grad[k] - fitted[k]
        for group, term in zip(terms, (lift * lift, lift * resid, resid * resid)):
            group.append(jnp.sum(term, axis=0, keepdims=True))
        terms[3].append(norms[k] / 16.0)
        terms[4].append(norms[2 + k] / 16.0)
    copy = pltpu.make_async_copy(buffer, both, sem)
    copy.start()
    lane = lax.broadcasted_iota(jnp.int32, (1, 128), 1)
    total = jnp.zeros((1, 128), jnp.float32)
    for n, term in enumerate(itertools.chain(*terms)):
        total = jnp.where(lane == n, jnp.sum(term, axis=1, keepdims=True), total)
    row[...] = total
    copy.wait()


def finished(own, ahead, far, behind, weights, lifted, fitted, norms):
    both = (2, *weights.shape)
    return pl.pallas_call(
        finish_kernel,
        in_specs=[pl.BlockSpec(memory_space=pltpu.VMEM)] * 8,
        out_specs=[
            pl.BlockSpec(memory_space=pltpu.VMEM),
            pl.BlockSpec(memory_space=pltpu.HBM),
        ],
        scratch_shapes=[pltpu.VMEM(both, jnp.float32), pltpu.SemaphoreType.DMA],
        out_shape=[
            jax.ShapeDtypeStruct((1, 128), jnp.float32),
            jax.ShapeDtypeStruct(both, jnp.float32),
        ],
        compiler_params=pltpu.CompilerParams(vmem_limit_bytes=8 * 2**20),
    )(own, ahead, far, behind, weights, lifted, fitted, norms)


def step_kernel(scalars, *refs):
    near, lifted, fitted, new_weights, update_out, copy = refs[:4], *refs[4:]
    row = jnp.sum(scalars[...], axis=0)
    lane = lax.broadcasted_iota(jnp.int32, row.shape, 1)
    terms = [
        jnp.sum(jnp.where(lane == n, row, 0.0), axis=1, keepdims=True) for n in range(10)
    ]
    total, ratios = 0.0, []
    for k in range(2):
        flat, cross, square, norm, length = terms[k::2]
        ratio = jnp.sqrt(norm) / jnp.sqrt(length + 1e-06)
        ratios.append(ratio)
        total = total + (flat + 2.0 * ratio * cross + ratio * ratio * square)
    scale = lax.rsqrt(jnp.maximum(total, 0.0) / (2.0 * D * QDIM) + 1e-06)
    for k in range(2):
        for a in range(4):
            step = lifted[k, a] + ratios[k] * (near[a][0, k] - fitted[k, a])
            update = scale * step
            new = near[a][1, k] - 0.02 * update
            copy[k, a] = new.astype(jnp.bfloat16)
            if a == 0:
                update_out[k] = update
                new_weights[k] = new


def stepped(scalars, near, lifted, fitted):
    own = near[0].shape[1:]
    return pl.pallas_call(
        step_kernel,
        in_specs=[pl.BlockSpec(memory_space=pltpu.VMEM)] * 7,
        out_specs=[pl.BlockSpec(memory_space=pltpu.VMEM)] * 3,
        out_shape=[
            jax.ShapeDtypeStruct(own, jnp.float32),
            jax.ShapeDtypeStruct(own, jnp.float32),
            jax.ShapeDtypeStruct(lifted.shape, jnp.bfloat16),
        ],
        compiler_params=pltpu.CompilerParams(vmem_limit_bytes=16 * 2**20),
    )(scalars, *near, lifted, fitted)


def products(left, right, factor):
    over_rows = (((0,), (0,)), ((), ()))
    grad = lax.dot_general(left, right, over_rows, preferred_element_type=jnp.float32)
    high = grad.astype(jnp.bfloat16)
    restored = lax.optimization_barrier(high).astype(jnp.float32)
    rest = (grad - restored).astype(jnp.bfloat16)
    low = 0.0
    for piece in (high, rest):
        low = low + lax.dot_general(factor, piece, over_rows, preferred_element_type=jnp.float32)
    return grad, low


def place_kernel(across, *refs):
    order, pieces, out, sems = refs[0], refs[1 : 1 + len(across)], refs[-2], refs[-1]
    copies = []
    for n, q in enumerate(across):
        for k in range(2):
            for j in range(4):
                start = pl.multiple_of(order[4 * j + q] * ROWS, ROWS)
                copies.append(
                    pltpu.make_async_copy(
                        pieces[n].at[k, j], out.at[k, pl.ds(start, ROWS)], sems.at[n, k, j]
                    )
                )
    for copy in copies:
        copy.start()
    for copy in copies:
        copy.wait()


def placed(order, across, pieces, out=None):
    count = len(across)
    olds = [] if out is None else [out]
    width = pieces[0].shape[-1]
    return pl.pallas_call(
        functools.partial(place_kernel, across),
        grid_spec=pltpu.PrefetchScalarGridSpec(
            num_scalar_prefetch=1,
            grid=(),
            in_specs=[pl.BlockSpec(memory_space=pltpu.VMEM)] * count
            + [pl.BlockSpec(memory_space=pl.ANY)] * len(olds),
            out_specs=pl.BlockSpec(memory_space=pl.ANY),
            scratch_shapes=[pltpu.SemaphoreType.DMA((count, 2, 4))],
        ),
        out_shape=jax.ShapeDtypeStruct((2, D, width), jnp.bfloat16),
        input_output_aliases={1 + count: 0} if olds else {},
        compiler_params=pltpu.CompilerParams(vmem_limit_bytes=8 * 2**20),
    )(order, *pieces, *olds)


def per_device(
    layer_inputs, output_cot, query_cot, head_outputs, weights, factors, first_moment, second_moment
):
    z, x, core = (lax.axis_index(a) for a in ("fs_0", "fs_1", "tp_1"))
    along = jnp.where(core == 0, x, z)
    across = jnp.where(core == 0, z, x)
    steps = jnp.arange(16, dtype=jnp.int32)
    there = (along + steps // 4) % 4
    beyond = (across + steps % 4) % 4
    order = jnp.where(core == 0, beyond * 4 + there, there * 4 + beyond)
    places = jnp.where(core == 0, steps % 4 * 4 + there, there * 4 + steps % 4)
    orders = (order, places)

    width = weights.shape[2]
    full, block = (4, ROWS, width), (2, ROWS, width)
    low_shape = (4, 2 * LOW_ROWS, width)

    grads, low_0 = products(layer_inputs, query_cot, factors[0])
    own, ahead, far, behind = small_call(spread_kernel, (full,) * 4, (order,))(grads)
    got = moved(far, True, 1)
    behind = moved(behind, True, -1)
    (ahead,) = small_call(add_kernel, (full,), aliases={0: 0})(ahead, got)
    parts = [own, moved(ahead, True, 1), behind]

    grads, low_1 = products(output_cot, head_outputs, factors[1])
    own, ahead, far, behind = small_call(spread_kernel, (full,) * 4, (order,))(grads)
    got = moved(far, True, -1)
    ahead = moved(ahead, True, 1)
    (behind,) = small_call(add_kernel, (full,), aliases={0: 0})(behind, got)
    parts += [own, ahead, moved(behind, True, -1)]

    low, *others = small_call(spread_low_kernel, (low_shape,) * 4, (places,))(low_0, low_1)
    (low,) = small_call(sum_kernel, (low_shape,))(low, *to_all(others, True))
    (quarter,) = small_call(sum_kernel, (low_shape,))(low, *to_all([low] * 3, False))
    quarters = [quarter, *to_all([quarter] * 3, True, -1)]
    own, ahead, far, behind = small_call(join_kernel, (block,) * 4)(*parts)
    across = to_all((ahead, far, behind), False)

    first, second, norms, lift_own, fit_own, lifted, fitted = moments(
        orders, quarters, factors, first_moment, second_moment
    )
    row, both = finished(own, *across, weights, lift_own, fit_own, norms)
    near = [both, *to_all([both] * 3, True, -1)]
    scalars = jnp.broadcast_to(row, (128, 1, 128))
    scalars = lax.all_to_all(scalars, ALL, split_axis=0, concat_axis=0, tiled=True)
    new_weights, update, copy = stepped(scalars, near, lifted, fitted)
    others = to_all([copy] * 3, False, -1)
    weight_copy = placed(order, (0,), [copy])
    weight_copy = placed(order, (1, 2, 3), others, weight_copy)
    return (new_weights, update, first, second, weight_copy)


def solution(mesh):
    finer = Mesh(mesh.devices.reshape(SIZES), ALL)
    tp = ("tp_0", "tp_1")
    in_specs = (
        P(FS, None),
        P(FS, None),
        P(FS, tp),
        P(FS, tp),
        P(None, FS, tp),
        P(),
        P(None, None, tp),
        P(None, None, tp),
    )
    out_specs = (
        P(None, FS, tp),
        P(None, FS, tp),
        P(None, None, tp),
        P(None, None, tp),
        P(None, None, tp),
    )

    return jax.shard_map(
        per_device, mesh=finer, in_specs=in_specs, out_specs=out_specs, check_vma=False
    )
```
